32 devices in a mesh: grp: 2 (over x), ep: 8 (over z, y), tp: 2 (over core).
Axes of the slice: x: 2, y: 2, z: 4, core: 2. Of those that a mesh axis runs over, the one named last changes fastest.
Arguments:
- tokens: bfloat16 [8192, 2048], P(('grp', 'ep', 'tp')), parts along dimension 0, may hold values from -6 to 6
- norm_gain: float32 [2048], replicated, may hold values from 0.1 to 1.9
- route_ids: int32 [8192, 2], P(('grp', 'ep', 'tp')), parts along dimension 0, may hold values from 0 to 7, as said below
- route_weights: float32 [8192, 2], P(('grp', 'ep', 'tp')), parts along dimension 0, may hold values from 0.1 to 1
- w_gate: bfloat16 [8, 2048, 512], P('ep', None, 'tp'), may hold values from -0.125 to 0.125
- w_up: bfloat16 [8, 2048, 512], P('ep', None, 'tp'), may hold values from -0.125 to 0.125
- w_down: bfloat16 [8, 512, 2048], P('ep', 'tp'), may hold values from -0.25 to 0.25
Outputs:
- mixed: bfloat16 [8192, 2048], P(('grp', 'ep', 'tp')), parts along dimension 0
The draws below stay inside these ranges and needn't reach their ends.
There are 2 independent parts, one for each index of `grp`. The reference program is written for one: setup_inputs(seed, part) draws one part's arguments, and reference() takes and returns one part's arrays. A program takes and returns all parts, laid end to end along the dimension named above; an argument that names none is the same for every part. Nothing has to cross between parts.
Inputs may be any that keep to these rules, and one draw needn't show every extreme that they name: `route_ids`: the 2 experts of a token are different and lie in one group of 2 consecutive experts. Among the tokens of one device (aligned blocks of 256 tokens) no expert is named more than 128 times, and in every such block some expert is named exactly 128 times.
All inputs are finite; a program needn't handle non-finite values.
Results may differ from the reference program's by a relative error of at most 0.007.
Values may be sent and summed in bfloat16 or wider, within the bound.
A program may use at most 128 MiB of HBM per device.

```python
import math
import jax
import jax.numpy as jnp
from jax import lax

D = 2048
FF = 512
GROUPS = 4
TOPK = 2
TOK_DEV = 256
EXPERTS = 8
EXP_GROUP = 2
CAP = 128
TOKENS = 4096


def route_block(block_key):
    subkeys = jax.random.split(block_key, 5)
    halfway = TOK_DEV // 2
    busiest = jax.random.randint(subkeys[0], (), 0, GROUPS)
    spare = halfway - (GROUPS - 1) * EXP_GROUP
    cut_points = jnp.sort(jax.random.randint(subkeys[1], (GROUPS - 2,), 0, spare + 1))
    bounds = jnp.concatenate([jnp.zeros((1,), jnp.int32), cut_points.astype(jnp.int32), jnp.full((1,), spare, jnp.int32)])
    group_sizes = jnp.concatenate([jnp.full((1,), halfway, jnp.int32), bounds[1:] - bounds[:-1] + EXP_GROUP])
    bound_ends = jnp.cumsum(group_sizes)
    starts = bound_ends - group_sizes
    position = jnp.arange(TOK_DEV, dtype=jnp.int32)
    group_rank = jnp.sum((position[:, None] >= bound_ends[None, :]).astype(jnp.int32), axis=1)
    within = position - starts[group_rank]
    group = (busiest + group_rank) % GROUPS
    offsets = jax.random.randint(subkeys[2], (GROUPS,), 0, EXP_GROUP)
    shifts = jax.random.randint(subkeys[3], (GROUPS,), 1, EXP_GROUP)
    first_pick = (within + offsets[group]) % EXP_GROUP
    second_pick = (first_pick + shifts[group]) % EXP_GROUP
    chosen = group[:, None] * EXP_GROUP + jnp.stack([first_pick, second_pick], axis=1)
    shuffle = jax.random.permutation(subkeys[4], TOK_DEV)
    return jnp.zeros((TOK_DEV, 2), jnp.int32).at[shuffle].set(chosen.astype(jnp.int32))


def draw_route_ids(key, part):
    block_keys = jax.random.split(jax.random.fold_in(key, 17), TOKENS // TOK_DEV)
    return jax.vmap(route_block)(block_keys).reshape(TOKENS, TOPK).astype(jnp.int32)


def levels(rng, dims, pieces, smallest, high):
    gain, own = 1.0, jax.random.fold_in(rng, 6)
    for dim, shards_of in pieces:
        steps = jnp.exp(jax.random.uniform(jax.random.fold_in(own, dim), (shards_of,), jnp.float32, smallest / len(pieces), high / len(pieces)))
        gain = gain * jnp.repeat(steps, dims[dim] // shards_of).reshape([-1 if axis == dim else 1 for axis in range(len(dims))])
    return gain


def gaussian(rng, dims, width, reach, pieces=(), held_as=jnp.bfloat16):
    loudness = levels(rng, dims, pieces, -0.22, 0.18) if pieces else 1.0
    result = jax.random.normal(rng, dims, jnp.float32) * width * loudness
    return jnp.minimum(jnp.maximum(result, -reach), reach).astype(held_as)


def setup_inputs(seed: int = 0, part: int = 0) -> dict:
    streams_of = jax.random.split(jax.random.key(seed), 8)
    own_keys = jax.random.split(jax.random.fold_in(streams_of[7], part), 8)
    return {
        "tokens": gaussian(own_keys[0], (TOKENS, D), 1.0, 6.0, ((0, 16),)),
        "norm_gain": jnp.clip(1.0 + 0.18 * jax.random.normal(streams_of[1], (D,), jnp.float32), 0.1, 1.9),
        "route_ids": draw_route_ids(jax.random.fold_in(jax.random.fold_in(streams_of[7], part), 71), part),
        "route_weights": jnp.clip(jnp.exp(math.log(1.0) - 2.3025851 * jax.random.uniform(own_keys[3], (TOKENS, TOPK), jnp.float32) ** levels(own_keys[3], (TOKENS, TOPK), ((0, 16),), -0.2, 0.2)), 0.1, 1.0),
        "w_gate": gaussian(streams_of[4], (EXPERTS, D, FF), D ** -0.5, 0.125, ((0, 8), (2, 2))),
        "w_up": gaussian(streams_of[5], (EXPERTS, D, FF), D ** -0.5, 0.125, ((0, 8), (2, 2))),
        "w_down": gaussian(streams_of[6], (EXPERTS, FF, D), FF ** -0.5, 0.25, ((0, 8), (1, 2))),
    }


epsilon = 1e-06

def reference(tokens, norm_gain, route_ids, route_weights, w_gate, w_up, w_down):
    floats = tokens.astype(jnp.float32)
    inverse = lax.rsqrt(lax.optimization_barrier(jnp.mean(floats * floats, axis=1, keepdims=True)) + epsilon)
    normed = (floats * inverse * norm_gain.astype(jnp.float32)).astype(jnp.bfloat16)
    blocks = TOKENS // TOK_DEV
    route_flat = route_ids.reshape(blocks, TOK_DEV * TOPK).astype(jnp.int32)
    onehot = (route_flat[:, :, None] == jnp.arange(EXPERTS, dtype=jnp.int32)[None, None, :]).astype(jnp.int32)
    slot_index = lax.optimization_barrier(jnp.sum((jnp.cumsum(onehot, axis=1) - onehot) * onehot, axis=2)).astype(jnp.int32)
    anchor = jnp.arange(blocks, dtype=jnp.int32)[:, None]
    position = ((route_flat * blocks + anchor) * CAP + slot_index).astype(jnp.int32)
    position = position.reshape(TOKENS, TOPK)
    buffer = jnp.zeros((EXPERTS * blocks * CAP, D), jnp.bfloat16)
    for column in range(TOPK):
        buffer = buffer.at[position[:, column]].set(normed)
    buffer = buffer.reshape(EXPERTS, blocks * CAP, D)

    def expert(inputs):
        batch_rows, gate_weight, up_weight, down_weight = inputs
        gate_pre = jnp.dot(batch_rows, gate_weight, preferred_element_type=jnp.float32)
        up_pre = jnp.dot(batch_rows, up_weight, preferred_element_type=jnp.float32)
        hidden = (jax.nn.silu(gate_pre) * up_pre).astype(jnp.bfloat16)
        return jnp.dot(hidden, down_weight, preferred_element_type=jnp.float32).astype(jnp.bfloat16)
    results = lax.map(expert, (buffer, w_gate, w_up, w_down)).reshape(EXPERTS * blocks * CAP, D)
    combined = jnp.zeros((TOKENS, D), jnp.float32)
    for column in range(TOPK):
        picked = results[position[:, column]].astype(jnp.float32)
        combined = combined + route_weights[:, column:column + 1].astype(jnp.float32) * picked
    return combined.astype(jnp.bfloat16)
```

```python
import functools

import jax
import jax.numpy as jnp
from jax import lax
from jax.experimental import pallas as pl
from jax.experimental.pallas import tpu as pltpu
from jax.sharding import PartitionSpec as P

GROUPS = 4
SPLIT = 2
MESH = pl.DeviceIdType.MESH


epsilon = 1e-06


def send_back(result):
    return lax.all_to_all(result, "ep", split_axis=0, concat_axis=0, tiled=True)


def general_layer(tokens, norm_gain, route_ids, route_weights, w_gate, w_up, w_down):
    row_count, features = tokens.shape
    top_count = route_ids.shape[1]
    local_experts = w_gate.shape[0]
    ep_size = lax.axis_size("ep")
    experts_all = ep_size * local_experts
    capacity = row_count * GROUPS // experts_all
    floats = tokens.astype(jnp.float32)
    inverse = lax.rsqrt(jnp.mean(floats * floats, axis=1, keepdims=True) + epsilon)
    normed = (floats * inverse * norm_gain).astype(jnp.bfloat16)
    flat_ids = route_ids.reshape(-1)
    onehot = (flat_ids[:, None] == jnp.arange(experts_all, dtype=jnp.int32)[None, :]).astype(
        jnp.int32
    )
    earlier = jnp.cumsum(onehot, axis=0) - onehot
    slot_index = jnp.sum(earlier * onehot, axis=1)
    target = (flat_ids * capacity + slot_index).reshape(row_count, top_count)
    outbound = jnp.zeros((experts_all * capacity, features), jnp.bfloat16)
    for column in range(top_count):
        outbound = outbound.at[target[:, column]].set(normed)
    outbound = outbound.reshape(ep_size, local_experts, capacity, features)
    full_gate, full_up, full_down = (
        lax.all_gather(w_gate, "tp", axis=2, tiled=True),
        lax.all_gather(w_up, "tp", axis=2, tiled=True),
        lax.all_gather(w_down, "tp", axis=1, tiled=True),
    )
    arrived = lax.all_to_all(outbound, "ep", split_axis=0, concat_axis=0, tiled=True)
    gate_pre = jnp.einsum("sjcd,jdf->sjcf", arrived, full_gate, preferred_element_type=jnp.float32)
    up_pre = jnp.einsum("sjcd,jdf->sjcf", arrived, full_up, preferred_element_type=jnp.float32)
    hidden = (jax.nn.silu(gate_pre) * up_pre).astype(jnp.bfloat16)
    result = jnp.einsum("sjcf,jfd->sjcd", hidden, full_down, preferred_element_type=jnp.float32)
    returned_rows = send_back(result.astype(jnp.bfloat16))
    returned_rows = returned_rows.reshape(experts_all * capacity, features)
    combined = jnp.zeros((row_count, features), jnp.float32)
    for column in range(top_count):
        picked = returned_rows[target[:, column]].astype(jnp.float32)
        combined = combined + route_weights[:, column : column + 1] * picked
    return combined.astype(jnp.bfloat16)


def group_kernel(
    members, parts, halves,
    tokens, gain, ids, weights, w_gate, w_up, w_down, out,
    normed, place, sent, taken, scales, scales_in, answers, returned,
    gate_all, up_all, down_all, hidden,
    own_sems, twin_s, twin_r, peer_s, peer_r, part_s, part_r,
    near_s, near_r, far_s, far_r, row_s, row_r, scale_s, scale_r, back_s, back_r,
):
    part, position, half = lax.axis_index("grp"), lax.axis_index("ep"), lax.axis_index("tp")
    level, member = position // members, position % members
    rows, features = tokens.shape
    slots = sent.shape[1]
    top_count = ids.shape[0]
    peer = {"ep": level * members + (members - 1 - member)}
    other_part = {"grp": parts - 1 - part}
    twin = {"tp": halves - 1 - half}

    def level_of(k):
        return {"ep": (level ^ k) * members + member}

    barrier = pltpu.get_barrier_semaphore()
    neighbours = [peer, other_part, twin] + [level_of(k) for k in range(1, GROUPS)]
    for device in neighbours:
        pl.semaphore_signal(barrier, inc=1, device_id=device, device_id_type=MESH)
    pl.semaphore_wait(barrier, len(neighbours))

    sources = (w_gate, w_up, w_down)
    stores = (gate_all, up_all, down_all)
    mine = member * halves + half
    theirs = (members - 1 - member) * halves + half

    def remote(src, dst, send, recv, device):
        return pltpu.make_async_remote_copy(
            src_ref=src, dst_ref=dst, send_sem=send, recv_sem=recv,
            device_id=device, device_id_type=MESH,
        )

    pieces = []
    for step in range(SPLIT):
        for tensor in range(3):
            size = sources[tensor].shape[0] // (parts * SPLIT)
            pieces.append((tensor, step, size))

    def span(index, which):
        tensor, step, size = pieces[index]
        start = pl.multiple_of((which * SPLIT + step) * size, size)
        return tensor, pl.ds(start, size)

    def peer_copy(index):
        tensor, window = span(index, part)
        return remote(
            sources[tensor].at[window], stores[tensor].at[mine, window],
            peer_s.at[index], peer_r.at[index], peer,
        )

    def spread_copy(index, which, send, recv, device):
        tensor, window = span(index, which)
        block = stores[tensor].at[theirs, window]
        return remote(block, block, send.at[index], recv.at[index], device)

    peer_copies = [peer_copy(index) for index in range(len(pieces))]
    part_copies = [spread_copy(i, part, part_s, part_r, other_part) for i in range(len(pieces))]
    near_copies = [spread_copy(i, part, near_s, near_r, twin) for i in range(len(pieces))]
    far_copies = [
        spread_copy(i, parts - 1 - part, far_s, far_r, twin) for i in range(len(pieces))
    ]
    for copy in peer_copies:
        copy.start()
    own_copies, twin_copies = [], []
    for tensor in range(3):
        own_copies.append(
            pltpu.make_async_copy(sources[tensor], stores[tensor].at[mine], own_sems.at[tensor])
        )
        twin_copies.append(
            remote(
                sources[tensor], stores[tensor].at[mine],
                twin_s.at[tensor], twin_r.at[tensor], twin,
            )
        )
    for copy in own_copies + twin_copies:
        copy.start()

    strip = 32

    def norm_strip(index, carry):
        window = pl.ds(pl.multiple_of(index * strip, strip), strip)
        floats = tokens[window, :].astype(jnp.float32)
        inverse = lax.rsqrt(jnp.mean(floats * floats, axis=1, keepdims=True) + epsilon)
        normed[window, :] = (floats * inverse * gain[...]).astype(jnp.bfloat16)
        return carry

    lax.fori_loop(0, rows // strip, norm_strip, 0)

    first = ids[0:1, :]
    group_row = first // members
    lane = lax.broadcasted_iota(jnp.int32, (8, rows), 0)
    mask = (jnp.broadcast_to(group_row, (8, rows)) == lane).astype(jnp.float32)
    before = (
        lax.broadcasted_iota(jnp.int32, (rows, rows), 0)
        < lax.broadcasted_iota(jnp.int32, (rows, rows), 1)
    ).astype(jnp.float32)
    ranks = jnp.dot(
        mask.astype(jnp.bfloat16), before.astype(jnp.bfloat16),
        preferred_element_type=jnp.float32,
    )
    slot_row = jnp.sum(ranks * mask, axis=0, keepdims=True).astype(jnp.int32)
    shares = jnp.zeros((8, rows), jnp.float32)
    for column in range(top_count):
        offset = ids[column : column + 1, :] - group_row * members
        chosen = jnp.broadcast_to(offset, (8, rows)) == lane
        shares = shares + jnp.where(
            chosen, jnp.broadcast_to(weights[column : column + 1, :], (8, rows)), 0.0
        )
    high = shares.astype(jnp.bfloat16)
    rest = shares - high.astype(jnp.float32)
    middle = rest.astype(jnp.bfloat16)
    low = (rest - middle.astype(jnp.float32)).astype(jnp.bfloat16)

    row_copies, scale_copies, back_copies = {}, {}, {}
    slot_iota = lax.broadcasted_iota(jnp.int32, (slots, rows), 0)
    order = [2, 3, 1, 0]
    for k in order:
        key = jnp.where(group_row == (level ^ k), slot_row, -1)
        spots = (jnp.broadcast_to(key, (slots, rows)) == slot_iota).astype(jnp.float32)
        spots = spots.astype(jnp.bfloat16)
        place[k * slots : (k + 1) * slots, :] = spots
        lanes = sum(
            lax.dot_general(
                piece, spots, (((1,), (1,)), ((), ())), preferred_element_type=jnp.float32
            )
            for piece in (high, middle, low)
        )
        packed = taken if k == 0 else sent
        (scales_in if k == 0 else scales)[k] = lanes
        packed[k] = jnp.dot(spots, normed[...], preferred_element_type=jnp.float32).astype(
            jnp.bfloat16
        )
        if k:
            row_copies[k] = remote(sent.at[k], taken.at[k], row_s.at[k], row_r.at[k], level_of(k))
            scale_copies[k] = remote(
                scales.at[k], scales_in.at[k], scale_s.at[k], scale_r.at[k], level_of(k)
            )
            row_copies[k].start()
            scale_copies[k].start()

    for index in range(len(pieces)):
        peer_copies[index].wait_recv()
        part_copies[index].start()
        near_copies[index].start()
        if index:
            part_copies[index - 1].wait_recv()
            far_copies[index - 1].start()
    part_copies[-1].wait_recv()
    far_copies[-1].start()
    for copy in own_copies:
        copy.wait()
    for copy in twin_copies + near_copies + far_copies:
        copy.wait_recv()

    width = gate_all.shape[2]
    diagonal = lax.broadcasted_iota(jnp.int32, (slots, slots), 0) == lax.broadcasted_iota(
        jnp.int32, (slots, slots), 1
    )
    tile = 512

    def work(k):
        for block in range(members * halves):
            lanes = scales_in[k][block // halves : block // halves + 1, :]
            scale = jnp.sum(
                jnp.where(diagonal, jnp.broadcast_to(lanes, (slots, slots)), 0.0),
                axis=1, keepdims=True,
            )
            gate = jnp.dot(taken[k], gate_all[block], preferred_element_type=jnp.float32)
            up = jnp.dot(taken[k], up_all[block], preferred_element_type=jnp.float32)
            hidden[:, block * width : (block + 1) * width] = (
                gate / (1.0 + jnp.exp(-gate)) * up * scale
            ).astype(jnp.bfloat16)
        for column in range(features // tile):
            window = slice(column * tile, (column + 1) * tile)
            total = jnp.zeros((slots, tile), jnp.float32)
            for block in range(members * halves):
                total += jnp.dot(
                    hidden[:, block * width : (block + 1) * width],
                    down_all[block, :, window],
                    preferred_element_type=jnp.float32,
                )
            if k:
                answers[k, :, window] = total.astype(jnp.bfloat16)
            else:
                returned[0, :, window] = total.astype(jnp.bfloat16)

    for k in (2, 3, 1, 0):
        if k:
            row_copies[k].wait_recv()
            scale_copies[k].wait_recv()
        work(k)
        if k:
            back_copies[k] = remote(
                answers.at[k], returned.at[k], back_s.at[k], back_r.at[k], level_of(k)
            )
            back_copies[k].start()

    for k in (1, 2, 3):
        back_copies[k].wait_recv()
    for column in range(features // tile):
        window = slice(column * tile, (column + 1) * tile)
        total = jnp.zeros((rows, tile), jnp.float32)
        for k in range(GROUPS):
            total += lax.dot_general(
                place[k * slots : (k + 1) * slots, :], returned[k, :, window],
                (((0,), (0,)), ((), ())), preferred_element_type=jnp.float32,
            )
        out[:, window] = total.astype(jnp.bfloat16)

    for copy in peer_copies + part_copies + near_copies + far_copies + twin_copies:
        copy.wait_send()
    for k in (1, 2, 3):
        row_copies[k].wait_send()
        scale_copies[k].wait_send()
        back_copies[k].wait_send()


def group_layer(members, tokens, norm_gain, route_ids, route_weights, w_gate, w_up, w_down):
    rows, features = tokens.shape
    parts, halves = lax.axis_size("grp"), lax.axis_size("tp")
    width = w_gate.shape[2]
    slots = rows // route_ids.shape[1]
    copies = 3 * SPLIT
    blocks = members * halves
    bf16, f32, dma = jnp.bfloat16, jnp.float32, pltpu.SemaphoreType.DMA
    vmem, anywhere = pl.BlockSpec(memory_space=pltpu.VMEM), pl.BlockSpec(memory_space=pl.ANY)
    return pl.pallas_call(
        functools.partial(group_kernel, members, parts, halves),
        out_shape=jax.ShapeDtypeStruct((rows, features), bf16),
        in_specs=[vmem] * 4 + [anywhere] * 3,
        out_specs=vmem,
        scratch_shapes=[
            pltpu.VMEM((rows, features), bf16),
            pltpu.VMEM((GROUPS * slots, rows), bf16),
            pltpu.VMEM((GROUPS, slots, features), bf16),
            pltpu.VMEM((GROUPS, slots, features), bf16),
            pltpu.VMEM((GROUPS, 8, slots), f32),
            pltpu.VMEM((GROUPS, 8, slots), f32),
            pltpu.VMEM((GROUPS, slots, features), bf16),
            pltpu.VMEM((GROUPS, slots, features), bf16),
            pltpu.VMEM((blocks, features, width), bf16),
            pltpu.VMEM((blocks, features, width), bf16),
            pltpu.VMEM((blocks, width, features), bf16),
            pltpu.VMEM((slots, blocks * width), bf16),
            dma((3,)), dma((3,)), dma((3,)),
        ]
        + [dma((copies,)) for _ in range(8)]
        + [dma((GROUPS,)) for _ in range(6)],
        compiler_params=pltpu.CompilerParams(
            collective_id=0, has_side_effects=True, vmem_limit_bytes=48 * 1024 * 1024
        ),
    )(
        tokens, norm_gain.reshape(1, features), route_ids.T, route_weights.T,
        w_gate[0], w_up[0], w_down[0],
    )


def solution(mesh):
    sizes = mesh.shape

    def per_device(tokens, norm_gain, route_ids, route_weights, w_gate, w_up, w_down):
        arguments = (tokens, norm_gain, route_ids, route_weights, w_gate, w_up, w_down)
        members = sizes["ep"] * w_gate.shape[0] // GROUPS
        paired = members == route_ids.shape[1] == sizes["grp"] == sizes["tp"] == 2
        if paired and w_gate.shape[0] == 1:
            return group_layer(members, *arguments)
        return general_layer(*arguments)

    in_specs = (
        P(("grp", "ep", "tp"), None),
        P(),
        P(("grp", "ep", "tp"), None),
        P(("grp", "ep", "tp"), None),
        P("ep", None, "tp"),
        P("ep", None, "tp"),
        P("ep", "tp", None),
    )
    out_specs = P(("grp", "ep", "tp"), None)
    return jax.shard_map(
        per_device, mesh=mesh, in_specs=in_specs, out_specs=out_specs, check_vma=False
    )
```

```python
import functools

import jax
import jax.numpy as jnp
from jax import lax
from jax.experimental import pallas as pl
from jax.experimental.pallas import tpu as pltpu
from jax.sharding import PartitionSpec as P

GROUPS = 4
SPLIT = 2
MESH = pl.DeviceIdType.MESH


epsilon = 1e-06


def send_back(result):
    return lax.all_to_all(result, "ep", split_axis=0, concat_axis=0, tiled=True)


def general_layer(tokens, norm_gain, route_ids, route_weights, w_gate, w_up, w_down):
    row_count, features = tokens.shape
    top_count = route_ids.shape[1]
    local_experts = w_gate.shape[0]
    ep_size = lax.axis_size("ep")
    experts_all = ep_size * local_experts
    capacity = row_count * GROUPS // experts_all
    floats = tokens.astype(jnp.float32)
    inverse = lax.rsqrt(jnp.mean(floats * floats, axis=1, keepdims=True) + epsilon)
    normed = (floats * inverse * norm_gain).astype(jnp.bfloat16)
    flat_ids = route_ids.reshape(-1)
    onehot = (flat_ids[:, None] == jnp.arange(experts_all, dtype=jnp.int32)[None, :]).astype(
        jnp.int32
    )
    earlier = jnp.cumsum(onehot, axis=0) - onehot
    slot_index = jnp.sum(earlier * onehot, axis=1)
    target = (flat_ids * capacity + slot_index).reshape(row_count, top_count)
    outbound = jnp.zeros((experts_all * capacity, features), jnp.bfloat16)
    for column in range(top_count):
        outbound = outbound.at[target[:, column]].set(normed)
    outbound = outbound.reshape(ep_size, local_experts, capacity, features)
    full_gate, full_up, full_down = (
        lax.all_gather(w_gate, "tp", axis=2, tiled=True),
        lax.all_gather(w_up, "tp", axis=2, tiled=True),
        lax.all_gather(w_down, "tp", axis=1, tiled=True),
    )
    arrived = lax.all_to_all(outbound, "ep", split_axis=0, concat_axis=0, tiled=True)
    gate_pre = jnp.einsum("sjcd,jdf->sjcf", arrived, full_gate, preferred_element_type=jnp.float32)
    up_pre = jnp.einsum("sjcd,jdf->sjcf", arrived, full_up, preferred_element_type=jnp.float32)
    hidden = (jax.nn.silu(gate_pre) * up_pre).astype(jnp.bfloat16)
    result = jnp.einsum("sjcf,jfd->sjcd", hidden, full_down, preferred_element_type=jnp.float32)
    returned_rows = send_back(result.astype(jnp.bfloat16))
    returned_rows = returned_rows.reshape(experts_all * capacity, features)
    combined = jnp.zeros((row_count, features), jnp.float32)
    for column in range(top_count):
        picked = returned_rows[target[:, column]].astype(jnp.float32)
        combined = combined + route_weights[:, column : column + 1] * picked
    return combined.astype(jnp.bfloat16)


def group_kernel(
    members, parts, halves,
    tokens, gain, ids, weights, w_gate, w_up, w_down, out,
    raw, ready, summed, place, sent, taken, scales, scales_in, answers, returned,
    gate_all, up_all, down_all, hidden,
    raw_sem, own_sems, twin_s, twin_r, peer_s, peer_r, part_s, part_r,
    near_s, near_r, far_s, far_r, row_s, row_r, scale_s, scale_r, back_s, back_r,
):
    part, position, half = lax.axis_index("grp"), lax.axis_index("ep"), lax.axis_index("tp")
    level, member = position // members, position % members
    rows, features = tokens.shape
    slots = sent.shape[1]
    top_count = ids.shape[0]
    peer = {"ep": level * members + (members - 1 - member)}
    other_part = {"grp": parts - 1 - part}
    twin = {"tp": halves - 1 - half}

    def level_of(k):
        return {"ep": (level ^ k) * members + member}

    raw_copy = pltpu.make_async_copy(tokens, raw, raw_sem)
    raw_copy.start()
    barrier = pltpu.get_barrier_semaphore()
    neighbours = [peer, other_part, twin] + [level_of(k) for k in range(1, GROUPS)]
    for device in neighbours:
        pl.semaphore_signal(barrier, inc=1, device_id=device, device_id_type=MESH)
    pl.semaphore_wait(barrier, len(neighbours))

    sources = (w_gate, w_up, w_down)
    stores = (gate_all, up_all, down_all)
    mine = member * halves + half
    theirs = (members - 1 - member) * halves + half

    def remote(src, dst, send, recv, device):
        return pltpu.make_async_remote_copy(
            src_ref=src, dst_ref=dst, send_sem=send, recv_sem=recv,
            device_id=device, device_id_type=MESH,
        )

    pieces = []
    for step in range(SPLIT):
        for tensor in range(3):
            size = sources[tensor].shape[0] // (parts * SPLIT)
            pieces.append((tensor, step, size))

    def span(index, which):
        tensor, step, size = pieces[index]
        start = pl.multiple_of((which * SPLIT + step) * size, size)
        return tensor, pl.ds(start, size)

    def peer_copy(index):
        tensor, window = span(index, part)
        return remote(
            sources[tensor].at[window], stores[tensor].at[mine, window],
            peer_s.at[index], peer_r.at[index], peer,
        )

    def spread_copy(index, which, send, recv, device):
        tensor, window = span(index, which)
        block = stores[tensor].at[theirs, window]
        return remote(block, block, send.at[index], recv.at[index], device)

    peer_copies = [peer_copy(index) for index in range(len(pieces))]
    part_copies = [spread_copy(i, part, part_s, part_r, other_part) for i in range(len(pieces))]
    near_copies = [spread_copy(i, part, near_s, near_r, twin) for i in range(len(pieces))]
    far_copies = [
        spread_copy(i, parts - 1 - part, far_s, far_r, twin) for i in range(len(pieces))
    ]
    for copy in peer_copies:
        copy.start()
    own_copies, twin_copies = [], []
    for tensor in range(3):
        own_copies.append(
            pltpu.make_async_copy(sources[tensor], stores[tensor].at[mine], own_sems.at[tensor])
        )
        twin_copies.append(
            remote(
                sources[tensor], stores[tensor].at[mine],
                twin_s.at[tensor], twin_r.at[tensor], twin,
            )
        )
    for copy in own_copies + twin_copies:
        copy.start()

    first = ids[0:1, :]
    group_row = first // members
    lane = lax.broadcasted_iota(jnp.int32, (8, rows), 0)
    mask = (jnp.broadcast_to(group_row, (8, rows)) == lane).astype(jnp.float32)
    before = (
        lax.broadcasted_iota(jnp.int32, (rows, rows), 0)
        < lax.broadcasted_iota(jnp.int32, (rows, rows), 1)
    ).astype(jnp.float32)
    ranks = jnp.dot(
        mask.astype(jnp.bfloat16), before.astype(jnp.bfloat16),
        preferred_element_type=jnp.float32,
    )
    slot_row = jnp.sum(ranks * mask, axis=0, keepdims=True).astype(jnp.int32)
    shares = jnp.zeros((8, rows), jnp.float32)
    for column in range(top_count):
        offset = ids[column : column + 1, :] - group_row * members
        chosen = jnp.broadcast_to(offset, (8, rows)) == lane
        shares = shares + jnp.where(
            chosen, jnp.broadcast_to(weights[column : column + 1, :], (8, rows)), 0.0
        )
    high = shares.astype(jnp.bfloat16)
    rest = shares - high.astype(jnp.float32)
    middle = rest.astype(jnp.bfloat16)
    low = (rest - middle.astype(jnp.float32)).astype(jnp.bfloat16)

    row_copies, scale_copies, back_copies = {}, {}, {}
    slot_iota = lax.broadcasted_iota(jnp.int32, (slots, rows), 0)
    raw_copy.wait()
    order = (2, 1, 3, 0)
    for k in order:
        key = jnp.where(group_row == (level ^ k), slot_row, -1)
        spots = (jnp.broadcast_to(key, (slots, rows)) == slot_iota).astype(jnp.float32)
        spots = spots.astype(jnp.bfloat16)
        place[k * slots : (k + 1) * slots, :] = spots
        lanes = sum(
            lax.dot_general(
                piece, spots, (((1,), (1,)), ((), ())), preferred_element_type=jnp.float32
            )
            for piece in (high, middle, low)
        )
        packed = taken if k == 0 else sent
        (scales_in if k == 0 else scales)[k] = lanes
        packed[k] = jnp.dot(spots, raw[...], preferred_element_type=jnp.float32).astype(
            jnp.bfloat16
        )
        if k:
            row_copies[k] = remote(sent.at[k], taken.at[k], row_s.at[k], row_r.at[k], level_of(k))
            scale_copies[k] = remote(
                scales.at[k], scales_in.at[k], scale_s.at[k], scale_r.at[k], level_of(k)
            )
            row_copies[k].start()
            scale_copies[k].start()

    for index in range(len(pieces)):
        peer_copies[index].wait_recv()
        part_copies[index].start()
        near_copies[index].start()
        if index:
            part_copies[index - 1].wait_recv()
            far_copies[index - 1].start()
    part_copies[-1].wait_recv()
    far_copies[-1].start()
    for copy in own_copies:
        copy.wait()
    for copy in twin_copies + near_copies + far_copies:
        copy.wait_recv()

    width = gate_all.shape[2]
    diagonal = lax.broadcasted_iota(jnp.int32, (slots, slots), 0) == lax.broadcasted_iota(
        jnp.int32, (slots, slots), 1
    )
    tile = 512

    strip = 32

    def work(k):
        def norm_strip(index, carry):
            window = pl.ds(pl.multiple_of(index * strip, strip), strip)
            floats = taken[k, window, :].astype(jnp.float32)
            inverse = lax.rsqrt(jnp.mean(floats * floats, axis=1, keepdims=True) + epsilon)
            ready[window, :] = (floats * inverse * gain[...]).astype(jnp.bfloat16)
            return carry

        lax.fori_loop(0, slots // strip, norm_strip, 0)
        for block in range(members * halves):
            lanes = scales_in[k][block // halves : block // halves + 1, :]
            scale = jnp.sum(
                jnp.where(diagonal, jnp.broadcast_to(lanes, (slots, slots)), 0.0),
                axis=1, keepdims=True,
            )
            gate = jnp.dot(ready[...], gate_all[block], preferred_element_type=jnp.float32)
            up = jnp.dot(ready[...], up_all[block], preferred_element_type=jnp.float32)
            hidden[:, block * width : (block + 1) * width] = (
                gate / (1.0 + jnp.exp(-gate)) * up * scale
            ).astype(jnp.bfloat16)
        for column in range(features // tile):
            window = slice(column * tile, (column + 1) * tile)
            total = jnp.zeros((slots, tile), jnp.float32)
            for block in range(members * halves):
                total += jnp.dot(
                    hidden[:, block * width : (block + 1) * width],
                    down_all[block, :, window],
                    preferred_element_type=jnp.float32,
                )
            if k:
                answers[k, :, window] = total.astype(jnp.bfloat16)
            else:
                returned[0, :, window] = total.astype(jnp.bfloat16)

    for k in order:
        if k:
            row_copies[k].wait_recv()
            scale_copies[k].wait_recv()
        work(k)
        if k:
            back_copies[k] = remote(
                answers.at[k], returned.at[k], back_s.at[k], back_r.at[k], level_of(k)
            )
            back_copies[k].start()

    def unpack(k, window):
        return lax.dot_general(
            place[k * slots : (k + 1) * slots, :], returned[k, :, window],
            (((0,), (0,)), ((), ())), preferred_element_type=jnp.float32,
        )

    tiles = [slice(start, start + tile) for start in range(0, features, tile)]
    for window in tiles:
        summed[:, window] = unpack(0, window)
    for k in order[:-1]:
        back_copies[k].wait_recv()
        for window in tiles:
            total = summed[:, window] + unpack(k, window)
            if k == order[-2]:
                out[:, window] = total.astype(jnp.bfloat16)
            else:
                summed[:, window] = total

    for copy in peer_copies + part_copies + near_copies + far_copies + twin_copies:
        copy.wait_send()
    for k in (1, 2, 3):
        row_copies[k].wait_send()
        scale_copies[k].wait_send()
        back_copies[k].wait_send()


def group_layer(members, tokens, norm_gain, route_ids, route_weights, w_gate, w_up, w_down):
    rows, features = tokens.shape
    parts, halves = lax.axis_size("grp"), lax.axis_size("tp")
    width = w_gate.shape[2]
    slots = rows // route_ids.shape[1]
    copies = 3 * SPLIT
    blocks = members * halves
    bf16, f32, dma = jnp.bfloat16, jnp.float32, pltpu.SemaphoreType.DMA
    vmem, anywhere = pl.BlockSpec(memory_space=pltpu.VMEM), pl.BlockSpec(memory_space=pl.ANY)
    return pl.pallas_call(
        functools.partial(group_kernel, members, parts, halves),
        out_shape=jax.ShapeDtypeStruct((rows, features), bf16),
        in_specs=[anywhere] + [vmem] * 3 + [anywhere] * 3,
        out_specs=vmem,
        scratch_shapes=[
            pltpu.VMEM((rows, features), bf16),
            pltpu.VMEM((slots, features), bf16),
            pltpu.VMEM((rows, features), f32),
            pltpu.VMEM((GROUPS * slots, rows), bf16),
            pltpu.VMEM((GROUPS, slots, features), bf16),
            pltpu.VMEM((GROUPS, slots, features), bf16),
            pltpu.VMEM((GROUPS, 8, slots), f32),
            pltpu.VMEM((GROUPS, 8, slots), f32),
            pltpu.VMEM((GROUPS, slots, features), bf16),
            pltpu.VMEM((GROUPS, slots, features), bf16),
            pltpu.VMEM((blocks, features, width), bf16),
            pltpu.VMEM((blocks, features, width), bf16),
            pltpu.VMEM((blocks, width, features), bf16),
            pltpu.VMEM((slots, blocks * width), bf16),
            dma, dma((3,)), dma((3,)), dma((3,)),
        ]
        + [dma((copies,)) for _ in range(8)]
        + [dma((GROUPS,)) for _ in range(6)],
        compiler_params=pltpu.CompilerParams(
            collective_id=0, has_side_effects=True, vmem_limit_bytes=63 * 1024 * 1024
        ),
    )(
        tokens, norm_gain.reshape(1, features), route_ids.T, route_weights.T,
        w_gate[0], w_up[0], w_down[0],
    )


def solution(mesh):
    sizes = mesh.shape

    def per_device(tokens, norm_gain, route_ids, route_weights, w_gate, w_up, w_down):
        arguments = (tokens, norm_gain, route_ids, route_weights, w_gate, w_up, w_down)
        members = sizes["ep"] * w_gate.shape[0] // GROUPS
        paired = members == route_ids.shape[1] == sizes["grp"] == sizes["tp"] == 2
        if paired and w_gate.shape[0] == 1:
            return group_layer(members, *arguments)
        return general_layer(*arguments)

    in_specs = (
        P(("grp", "ep", "tp"), None),
        P(),
        P(("grp", "ep", "tp"), None),
        P(("grp", "ep", "tp"), None),
        P("ep", None, "tp"),
        P("ep", None, "tp"),
        P("ep", "tp", None),
    )
    out_specs = P(("grp", "ep", "tp"), None)
    return jax.shard_map(
        per_device, mesh=mesh, in_specs=in_specs, out_specs=out_specs, check_vma=False
    )
```

```python
import functools

import jax
import jax.numpy as jnp
from jax import lax
from jax.experimental import pallas as pl
from jax.experimental.pallas import tpu as pltpu
from jax.sharding import PartitionSpec as P

GROUPS = 4
SPLIT = 4
MESH = pl.DeviceIdType.MESH


epsilon = 1e-06


def send_back(result):
    return lax.all_to_all(result, "ep", split_axis=0, concat_axis=0, tiled=True)


def general_layer(tokens, norm_gain, route_ids, route_weights, w_gate, w_up, w_down):
    row_count, features = tokens.shape
    top_count = route_ids.shape[1]
    local_experts = w_gate.shape[0]
    ep_size = lax.axis_size("ep")
    experts_all = ep_size * local_experts
    capacity = row_count * GROUPS // experts_all
    floats = tokens.astype(jnp.float32)
    inverse = lax.rsqrt(jnp.mean(floats * floats, axis=1, keepdims=True) + epsilon)
    normed = (floats * inverse * norm_gain).astype(jnp.bfloat16)
    flat_ids = route_ids.reshape(-1)
    onehot = (flat_ids[:, None] == jnp.arange(experts_all, dtype=jnp.int32)[None, :]).astype(
        jnp.int32
    )
    earlier = jnp.cumsum(onehot, axis=0) - onehot
    slot_index = jnp.sum(earlier * onehot, axis=1)
    target = (flat_ids * capacity + slot_index).reshape(row_count, top_count)
    outbound = jnp.zeros((experts_all * capacity, features), jnp.bfloat16)
    for column in range(top_count):
        outbound = outbound.at[target[:, column]].set(normed)
    outbound = outbound.reshape(ep_size, local_experts, capacity, features)
    full_gate, full_up, full_down = (
        lax.all_gather(w_gate, "tp", axis=2, tiled=True),
        lax.all_gather(w_up, "tp", axis=2, tiled=True),
        lax.all_gather(w_down, "tp", axis=1, tiled=True),
    )
    arrived = lax.all_to_all(outbound, "ep", split_axis=0, concat_axis=0, tiled=True)
    gate_pre = jnp.einsum("sjcd,jdf->sjcf", arrived, full_gate, preferred_element_type=jnp.float32)
    up_pre = jnp.einsum("sjcd,jdf->sjcf", arrived, full_up, preferred_element_type=jnp.float32)
    hidden = (jax.nn.silu(gate_pre) * up_pre).astype(jnp.bfloat16)
    result = jnp.einsum("sjcf,jfd->sjcd", hidden, full_down, preferred_element_type=jnp.float32)
    returned_rows = send_back(result.astype(jnp.bfloat16))
    returned_rows = returned_rows.reshape(experts_all * capacity, features)
    combined = jnp.zeros((row_count, features), jnp.float32)
    for column in range(top_count):
        picked = returned_rows[target[:, column]].astype(jnp.float32)
        combined = combined + route_weights[:, column : column + 1] * picked
    return combined.astype(jnp.bfloat16)


def group_kernel(
    members, parts, halves,
    tokens, gain, ids, weights, w_gate, w_up, w_down, out,
    raw, ready, summed, final, place, sent, taken, scales, scales_in, answers, returned,
    gate_all, up_all, down_all, hidden,
    raw_sem, out_sems, own_sems, twin_s, twin_r, peer_s, peer_r, part_s, part_r,
    near_s, near_r, far_s, far_r, row_s, row_r, scale_s, scale_r, back_s, back_r,
):
    part, position, half = lax.axis_index("grp"), lax.axis_index("ep"), lax.axis_index("tp")
    level, member = position // members, position % members
    rows, features = tokens.shape
    slots = sent.shape[1]
    top_count = ids.shape[0]
    peer = {"ep": level * members + (members - 1 - member)}
    other_part = {"grp": parts - 1 - part}
    twin = {"tp": halves - 1 - half}

    def level_of(k):
        return {"ep": (level ^ k) * members + member}

    raw_copy = pltpu.make_async_copy(tokens, raw, raw_sem)
    raw_copy.start()
    barrier = pltpu.get_barrier_semaphore()
    neighbours = [peer, other_part, twin] + [level_of(k) for k in range(1, GROUPS)]
    for device in neighbours:
        pl.semaphore_signal(barrier, inc=1, device_id=device, device_id_type=MESH)

    sources = (w_gate, w_up, w_down)
    stores = (gate_all, up_all, down_all)
    mine = member * halves + half
    theirs = (members - 1 - member) * halves + half

    def remote(src, dst, send, recv, device):
        return pltpu.make_async_remote_copy(
            src_ref=src, dst_ref=dst, send_sem=send, recv_sem=recv,
            device_id=device, device_id_type=MESH,
        )

    pieces = []
    for step in range(SPLIT):
        for tensor in range(3):
            size = sources[tensor].shape[0] // (parts * SPLIT)
            pieces.append((tensor, step, size))

    def span(index, which):
        tensor, step, size = pieces[index]
        start = pl.multiple_of((which * SPLIT + step) * size, size)
        return tensor, pl.ds(start, size)

    def peer_copy(index):
        tensor, window = span(index, part)
        return remote(
            sources[tensor].at[window], stores[tensor].at[mine, window],
            peer_s.at[index], peer_r.at[index], peer,
        )

    def spread_copy(index, which, send, recv, device):
        tensor, window = span(index, which)
        block = stores[tensor].at[theirs, window]
        return remote(block, block, send.at[index], recv.at[index], device)

    peer_copies = [peer_copy(index) for index in range(len(pieces))]
    part_copies = [spread_copy(i, part, part_s, part_r, other_part) for i in range(len(pieces))]
    near_copies = [spread_copy(i, part, near_s, near_r, twin) for i in range(len(pieces))]
    far_copies = [
        spread_copy(i, parts - 1 - part, far_s, far_r, twin) for i in range(len(pieces))
    ]
    own_copies, twin_copies = [], []
    for tensor in range(3):
        own_copies.append(
            pltpu.make_async_copy(sources[tensor], stores[tensor].at[mine], own_sems.at[tensor])
        )
        twin_copies.append(
            remote(
                sources[tensor], stores[tensor].at[mine],
                twin_s.at[tensor], twin_r.at[tensor], twin,
            )
        )
    first = ids[0:1, :]
    group_row = first // members
    lane = lax.broadcasted_iota(jnp.int32, (8, rows), 0)
    mask = (jnp.broadcast_to(group_row, (8, rows)) == lane).astype(jnp.float32)
    before = (
        lax.broadcasted_iota(jnp.int32, (rows, rows), 0)
        < lax.broadcasted_iota(jnp.int32, (rows, rows), 1)
    ).astype(jnp.float32)
    ranks = jnp.dot(
        mask.astype(jnp.bfloat16), before.astype(jnp.bfloat16),
        preferred_element_type=jnp.float32,
    )
    slot_row = jnp.sum(ranks * mask, axis=0, keepdims=True).astype(jnp.int32)
    shares = jnp.zeros((8, rows), jnp.float32)
    for column in range(top_count):
        offset = ids[column : column + 1, :] - group_row * members
        chosen = jnp.broadcast_to(offset, (8, rows)) == lane
        shares = shares + jnp.where(
            chosen, jnp.broadcast_to(weights[column : column + 1, :], (8, rows)), 0.0
        )
    high = shares.astype(jnp.bfloat16)
    rest = shares - high.astype(jnp.float32)
    middle = rest.astype(jnp.bfloat16)
    low = (rest - middle.astype(jnp.float32)).astype(jnp.bfloat16)

    row_copies, scale_copies, back_copies = {}, {}, {}
    slot_iota = lax.broadcasted_iota(jnp.int32, (slots, rows), 0)
    order = (2, 1, 3, 0)
    pl.semaphore_wait(barrier, len(neighbours))
    for copy in peer_copies:
        copy.start()
    raw_copy.wait()
    for k in order:
        key = jnp.where(group_row == (level ^ k), slot_row, -1)
        spots = (jnp.broadcast_to(key, (slots, rows)) == slot_iota).astype(jnp.float32)
        spots = spots.astype(jnp.bfloat16)
        place[k * slots : (k + 1) * slots, :] = spots
        lanes = sum(
            lax.dot_general(
                piece, spots, (((1,), (1,)), ((), ())), preferred_element_type=jnp.float32
            )
            for piece in (high, middle, low)
        )
        packed = taken if k == 0 else sent
        (scales_in if k == 0 else scales)[k] = lanes
        packed[k] = jnp.dot(spots, raw[...], preferred_element_type=jnp.float32).astype(
            jnp.bfloat16
        )
        if k:
            row_copies[k] = remote(sent.at[k], taken.at[k], row_s.at[k], row_r.at[k], level_of(k))
            scale_copies[k] = remote(
                scales.at[k], scales_in.at[k], scale_s.at[k], scale_r.at[k], level_of(k)
            )
            row_copies[k].start()
            scale_copies[k].start()
        if k == order[0]:
            for copy in own_copies + twin_copies:
                copy.start()

    for index in range(len(pieces)):
        peer_copies[index].wait_recv()
        part_copies[index].start()
        near_copies[index].start()
        if index:
            part_copies[index - 1].wait_recv()
            far_copies[index - 1].start()
    part_copies[-1].wait_recv()
    far_copies[-1].start()

    width = gate_all.shape[2]
    diagonal = lax.broadcasted_iota(jnp.int32, (slots, slots), 0) == lax.broadcasted_iota(
        jnp.int32, (slots, slots), 1
    )
    tile = features // GROUPS

    strip = 32

    def norm(k):
        def norm_strip(index, carry):
            window = pl.ds(pl.multiple_of(index * strip, strip), strip)
            floats = taken[k, window, :].astype(jnp.float32)
            inverse = lax.rsqrt(jnp.mean(floats * floats, axis=1, keepdims=True) + epsilon)
            ready[window, :] = (floats * inverse * gain[...]).astype(jnp.bfloat16)
            return carry

        lax.fori_loop(0, slots // strip, norm_strip, 0)

    def widen(k, owner):
        lanes = scales_in[k, pl.ds(owner, 1), :]
        scale = jnp.sum(
            jnp.where(diagonal, jnp.broadcast_to(lanes, (slots, slots)), 0.0),
            axis=1, keepdims=True,
        )
        for side in range(halves):
            block = owner * halves + side
            gate = jnp.dot(ready[...], gate_all[block], preferred_element_type=jnp.float32)
            up = jnp.dot(ready[...], up_all[block], preferred_element_type=jnp.float32)
            hidden[:, pl.ds(pl.multiple_of(block * width, width), width)] = (
                gate / (1.0 + jnp.exp(-gate)) * up * scale
            ).astype(jnp.bfloat16)

    def narrow(k):
        for column in range(features // tile):
            window = slice(column * tile, (column + 1) * tile)
            total = jnp.zeros((slots, tile), jnp.float32)
            for block in range(members * halves):
                total += jnp.dot(
                    hidden[:, block * width : (block + 1) * width],
                    down_all[block, :, window],
                    preferred_element_type=jnp.float32,
                )
            if k:
                answers[k, :, window] = total.astype(jnp.bfloat16)
            else:
                returned[0, :, window] = total.astype(jnp.bfloat16)

    for copy in own_copies:
        copy.wait()
    for copy in twin_copies:
        copy.wait_recv()
    for k in order:
        if k:
            row_copies[k].wait_recv()
            scale_copies[k].wait_recv()
        norm(k)
        widen(k, member)
        if k == order[0]:
            for copy in near_copies + far_copies:
                copy.wait_recv()
        widen(k, members - 1 - member)
        narrow(k)
        if k:
            back_copies[k] = remote(
                answers.at[k], returned.at[k], back_s.at[k], back_r.at[k], level_of(k)
            )
            back_copies[k].start()

    def unpack(k, window):
        return lax.dot_general(
            place[k * slots : (k + 1) * slots, :], returned[k, :, window],
            (((0,), (0,)), ((), ())), preferred_element_type=jnp.float32,
        )

    tiles = [slice(start, start + tile) for start in range(0, features, tile)]
    for window in tiles:
        summed[:, window] = unpack(0, window)
    out_copies = []
    for k in order[:-1]:
        back_copies[k].wait_recv()
        for window in tiles:
            total = summed[:, window] + unpack(k, window)
            if k == order[-2]:
                final[:, window] = total.astype(jnp.bfloat16)
                copy = pltpu.make_async_copy(
                    final.at[:, window], out.at[:, window], out_sems.at[window.start // tile]
                )
                copy.start()
                out_copies.append(copy)
            else:
                summed[:, window] = total

    for copy in peer_copies + part_copies + near_copies + far_copies + twin_copies:
        copy.wait_send()
    for k in (1, 2, 3):
        row_copies[k].wait_send()
        scale_copies[k].wait_send()
        back_copies[k].wait_send()
    for copy in out_copies:
        copy.wait()


def group_layer(members, tokens, norm_gain, route_ids, route_weights, w_gate, w_up, w_down):
    rows, features = tokens.shape
    parts, halves = lax.axis_size("grp"), lax.axis_size("tp")
    width = w_gate.shape[2]
    slots = rows // route_ids.shape[1]
    copies = 3 * SPLIT
    blocks = members * halves
    bf16, f32, dma = jnp.bfloat16, jnp.float32, pltpu.SemaphoreType.DMA
    vmem, anywhere = pl.BlockSpec(memory_space=pltpu.VMEM), pl.BlockSpec(memory_space=pl.ANY)
    return pl.pallas_call(
        functools.partial(group_kernel, members, parts, halves),
        out_shape=jax.ShapeDtypeStruct((rows, features), bf16),
        in_specs=[anywhere] + [vmem] * 3 + [anywhere] * 3,
        out_specs=anywhere,
        scratch_shapes=[
            pltpu.VMEM((rows, features), bf16),
            pltpu.VMEM((slots, features), bf16),
            pltpu.VMEM((rows, features), f32),
            pltpu.VMEM((rows, features), bf16),
            pltpu.VMEM((GROUPS * slots, rows), bf16),
            pltpu.VMEM((GROUPS, slots, features), bf16),
            pltpu.VMEM((GROUPS, slots, features), bf16),
            pltpu.VMEM((GROUPS, 8, slots), f32),
            pltpu.VMEM((GROUPS, 8, slots), f32),
            pltpu.VMEM((GROUPS, slots, features), bf16),
            pltpu.VMEM((GROUPS, slots, features), bf16),
            pltpu.VMEM((blocks, features, width), bf16),
            pltpu.VMEM((blocks, features, width), bf16),
            pltpu.VMEM((blocks, width, features), bf16),
            pltpu.VMEM((slots, blocks * width), bf16),
            dma, dma((GROUPS,)), dma((3,)), dma((3,)), dma((3,)),
        ]
        + [dma((copies,)) for _ in range(8)]
        + [dma((GROUPS,)) for _ in range(6)],
        compiler_params=pltpu.CompilerParams(
            collective_id=0, has_side_effects=True, vmem_limit_bytes=63 * 1024 * 1024
        ),
    )(
        tokens, norm_gain.reshape(1, features), route_ids.T, route_weights.T,
        w_gate[0], w_up[0], w_down[0],
    )


def solution(mesh):
    sizes = mesh.shape

    def per_device(tokens, norm_gain, route_ids, route_weights, w_gate, w_up, w_down):
        arguments = (tokens, norm_gain, route_ids, route_weights, w_gate, w_up, w_down)
        members = sizes["ep"] * w_gate.shape[0] // GROUPS
        paired = members == route_ids.shape[1] == sizes["grp"] == sizes["tp"] == 2
        if paired and w_gate.shape[0] == 1:
            return group_layer(members, *arguments)
        return general_layer(*arguments)

    in_specs = (
        P(("grp", "ep", "tp"), None),
        P(),
        P(("grp", "ep", "tp"), None),
        P(("grp", "ep", "tp"), None),
        P("ep", None, "tp"),
        P("ep", None, "tp"),
        P("ep", "tp", None),
    )
    out_specs = P(("grp", "ep", "tp"), None)
    return jax.shard_map(
        per_device, mesh=mesh, in_specs=in_specs, out_specs=out_specs, check_vma=False
    )
```
